32 devices in a mesh: fs: 8 (over z, x), tp: 4 (over y, core).
Axes of the slice: x: 2, y: 2, z: 4, core: 2. Of those that a mesh axis runs over, the one named last changes fastest.
Arguments:
- tokens: bfloat16 [4096, 2048], P('fs', 'tp'), may hold values from -6 to 6
- pre_gain: float32 [2048], P('fs'), may hold values from 0.1 to 1.9
- gate_weight: float32 [2048, 6144], P('fs', 'tp'), may hold values from -0.125 to 0.125
- up_weight: float32 [2048, 6144], P('fs', 'tp'), may hold values from -0.125 to 0.125
- down_weight: float32 [2048, 6144], P('fs', 'tp'), may hold values from -0.078125 to 0.078125
- post_gain: float32 [2048], P('tp'), may hold values from 0.1 to 1.9
Outputs:
- result: bfloat16 [4096, 2048], P('fs', 'tp')
- gate_ready: bfloat16 [2048, 6144], P(None, 'tp')
- up_ready: bfloat16 [2048, 6144], P(None, 'tp')
- down_ready: bfloat16 [2048, 6144], P(None, 'tp')
The draws below stay inside these ranges and needn't reach their ends.
All inputs are finite; a program needn't handle non-finite values.
Results may differ from the reference program's by a relative error of at most 0.015.
Values may be sent and summed in bfloat16 or wider, within the bound.
A program may use at most 128 MiB of HBM per device.

```python
import jax
import jax.numpy as jnp
from jax import lax

D = 2048
FF = 6144
TOKENS = 4096


def levels(rng, shape, pieces, smallest, top_value):
    def one(position, blocks):
        heights = jax.random.uniform(jax.random.fold_in(jax.random.fold_in(rng, 6), position), (blocks,), jnp.float32, smallest / len(pieces), top_value / len(pieces))
        return jnp.repeat(jnp.exp(heights), shape[position] // blocks).reshape((-1,) + (1,) * (len(shape) - position - 1))

    loudness = one(*pieces[0])
    for cut in pieces[1:]:
        loudness = loudness * one(*cut)
    return loudness


def bell_draw(stream_key, extent, spread, reach, cuts=(), kind=jnp.bfloat16):
    drawn = jax.random.normal(stream_key, extent, jnp.float32) * spread
    if len(cuts) > 0:
        drawn = levels(stream_key, extent, cuts, -0.22, 0.18) * drawn
    return jnp.clip(drawn, min=-reach, max=reach).astype(kind)


def setup_inputs(seed: int = 0) -> dict:
    keys = jax.random.split(jax.random.key(seed), 7)
    return {
        "tokens": bell_draw(keys[0], (TOKENS, D), 1.0, 6.0, ((0, 8), (1, 4))),
        "pre_gain": jnp.clip(1.0 + 0.18 * jax.random.normal(keys[1], (D,), jnp.float32), 0.1, 1.9),
        "gate_weight": bell_draw(keys[2], (D, FF), D ** -0.5, 0.125, ((0, 8), (1, 4)), jnp.float32),
        "up_weight": bell_draw(keys[3], (D, FF), D ** -0.5, 0.125, ((0, 8), (1, 4)), jnp.float32),
        "down_weight": bell_draw(keys[4], (D, FF), FF ** -0.5, 0.078125, ((0, 8), (1, 4)), jnp.float32),
        "post_gain": jnp.clip(1.0 + 0.18 * jax.random.normal(keys[5], (D,), jnp.float32), 0.1, 1.9),
    }


EPS = 1e-06

def reference(tokens, pre_gain, gate_weight, up_weight, down_weight, post_gain):
    gate_ready = (pre_gain[:, None] * gate_weight).astype(jnp.bfloat16)
    up_ready = (pre_gain[:, None] * up_weight).astype(jnp.bfloat16)
    down_ready = down_weight.astype(jnp.bfloat16)
    widened = tokens.astype(jnp.float32)
    normalized = (widened * lax.rsqrt(lax.optimization_barrier(jnp.mean(widened * widened, axis=1, keepdims=True)) + EPS)).astype(jnp.bfloat16)
    gate = jnp.dot(normalized, gate_ready, preferred_element_type=jnp.float32)
    up = jnp.dot(normalized, up_ready, preferred_element_type=jnp.float32)
    hidden = (jax.nn.silu(gate) * up).astype(jnp.bfloat16)
    mixed = lax.dot_general(hidden, down_ready, (((1,), (1,)), ((), ())), preferred_element_type=jnp.float32)
    scaling = lax.rsqrt(lax.optimization_barrier(jnp.mean(mixed * mixed, axis=1, keepdims=True)) + EPS)
    result = (mixed * scaling * post_gain[None, :]).astype(jnp.bfloat16)
    return (result, gate_ready, up_ready, down_ready)
```

```python
import functools

import jax
import jax.numpy as jnp
from jax import lax
from jax.experimental import pallas as pl
from jax.experimental.pallas import tpu as pltpu
from jax.sharding import PartitionSpec as P

EPS = 1e-06
MESH = pl.DeviceIdType.MESH
Q_PART, P_PART = 0, 1
UP, DOWN, RIGHT, LEFT = 0, 1, 2, 3


def split_rows(depth, lines, cols):
    if cols == 1 or lines == 1:
        return [0, 0, 0]
    share = ((cols - 1) * lines - (lines - 1)) / (2 * (lines - 1) * (cols - 1))
    share = min(max(share, 0.0), 1.0)
    units = min(int(round(3 * depth * share / 16)), 3 * (depth // 16))
    return [16 * (units // 3 + (1 if m >= 3 - units % 3 else 0)) for m in range(3)]


def kernel(
    fs, tp, lines, cols, first_rows,
    tokens, gate_own, up_own, down_own, post_gain,
    result, gate_out, up_out, down_out,
    held, whole, normed, gate, hidden, part, parts_in, squares, squares_in,
    send_sem, recv_sem, own_sem, out_sem, tok_send, tok_recv, tok_own,
    rs_send, rs_recv, sq_send, sq_recv,
):
    owns, outs = (gate_own, up_own, down_own), (gate_out, up_out, down_out)
    depth, width = gate_own.shape
    rows, block = tokens.shape
    me_fs, me = lax.axis_index("fs"), lax.axis_index("tp")
    z, x = me_fs // cols, lax.rem(me_fs, cols)
    finals = []

    sides = {
        UP: (z < lines - 1, me_fs + cols),
        DOWN: (z > 0, me_fs - cols),
        RIGHT: (x < cols - 1, me_fs + 1),
        LEFT: (x > 0, me_fs - 1),
    }
    peers = [lax.rem(me + j, tp) for j in range(1, tp)]

    def piece(m, which, shard):
        start, size = (0, first_rows[m]) if which == P_PART else (first_rows[m], depth - first_rows[m])
        return held.at[m, pl.ds(pl.multiple_of(shard * depth + start, 16), size), :]

    def describe(m, which, shard, side, target):
        ref = piece(m, which, shard)
        return pltpu.make_async_remote_copy(
            src_ref=ref, dst_ref=ref,
            send_sem=send_sem.at[m, which, shard, side],
            recv_sem=recv_sem.at[m, which, shard],
            device_id={"fs": target, "tp": me}, device_id_type=MESH,
        )

    def empty(m, which):
        return (first_rows[m] if which == P_PART else depth - first_rows[m]) == 0

    def send(m, which, shard, side, extra=None):
        if empty(m, which):
            return
        there, target = sides[side]
        cond = there if extra is None else jnp.logical_and(there, extra)

        @pl.when(cond)
        def _():
            describe(m, which, shard, side, target).start()

        def finish():
            @pl.when(cond)
            def _():
                describe(m, which, shard, side, target).wait_send()

        finals.append(finish)

    def arrive(m, which, shard, cond):
        if empty(m, which):
            return

        @pl.when(cond)
        def _():
            describe(m, which, shard, 0, lax.rem(me_fs + 1, fs)).wait_recv()

    barrier = pltpu.get_barrier_semaphore()
    for side in sides:
        there, target = sides[side]

        @pl.when(there)
        def _():
            pl.semaphore_signal(barrier, inc=1, device_id={"fs": target, "tp": me}, device_id_type=MESH)

    for peer in peers:
        pl.semaphore_signal(barrier, inc=1, device_id={"fs": me_fs, "tp": peer}, device_id_type=MESH)

    own_copies = [pltpu.make_async_copy(owns[m], held.at[m, pl.ds(pl.multiple_of(me_fs * depth, 16), depth), :], own_sem.at[m]) for m in range(3)]
    for c in own_copies:
        c.start()
    own_tokens = pltpu.make_async_copy(tokens, whole.at[me], tok_own)
    own_tokens.start()
    pl.semaphore_wait(barrier, tp - 1 + sum(there.astype(jnp.int32) for there, _ in sides.values()))

    def token_copy(j):
        return pltpu.make_async_remote_copy(
            src_ref=tokens, dst_ref=whole.at[me], send_sem=tok_send.at[j], recv_sem=tok_recv.at[j],
            device_id={"fs": me_fs, "tp": peers[j]}, device_id_type=MESH,
        )

    def start_own(m):
        own_copies[m].wait()
        for which in (P_PART, Q_PART):
            for side in (RIGHT, LEFT):
                send(m, which, me_fs, side)
            if which == Q_PART:
                for side in (UP, DOWN):
                    send(m, which, me_fs, side)

    start_own(0)
    for j in range(tp - 1):
        token_copy(j).start()

    def normalize():
        own_tokens.wait()
        for j in range(tp - 1):
            token_copy(j).wait_recv()
        step = 64

        @pl.loop(0, rows // step)
        def _(i):
            here = pl.ds(pl.multiple_of(i * step, step), step)
            total = jnp.zeros((step, 1), jnp.float32)
            for t in range(tp):
                v = whole[t, here, :].astype(jnp.float32)
                total = total + jnp.sum(v * v, axis=1, keepdims=True)
            scale = lax.rsqrt(total / (tp * block) + EPS)
            for t in range(tp):
                v = whole[t, here, :].astype(jnp.float32)
                normed[here, t * block:(t + 1) * block] = (v * scale).astype(jnp.bfloat16)

    def along_x(m, which, line, cond=None):
        for r in range(cols - 1):
            for side, column in ((RIGHT, x - 1 - r), (LEFT, x + 1 + r)):
                there = jnp.logical_and(column >= 0, column < cols)
                if cond is not None:
                    there = jnp.logical_and(there, cond)
                arrive(m, which, line * cols + column, there)
                if r < cols - 2:
                    send(m, which, line * cols + column, side, there)

    def along_z(m, which, s, columns):
        for side, line in ((UP, z - 1 - s), (DOWN, z + 1 + s)):
            there = jnp.logical_and(line >= 0, line < lines)
            for column in columns:
                shard = line * cols + column
                arrive(m, which, shard, there)
                if s < lines - 2:
                    send(m, which, shard, side, there)
                if which == Q_PART:
                    send(m, which, shard, RIGHT, there)
                    send(m, which, shard, LEFT, there)

    def first_half(m):
        for s in range(lines - 1):
            along_z(m, Q_PART, s, [x])
        along_x(m, P_PART, z)
        for column in range(cols):
            for side in (UP, DOWN):
                send(m, P_PART, z * cols + column, side)

    def whole_out(m):
        return pltpu.make_async_copy(held.at[m], outs[m], out_sem.at[m])

    tile = 256
    for m in range(2):
        first_half(m)
        for s in range(lines - 1):
            along_z(m, P_PART, s, range(cols))
        start_own(m + 1)
        if m == 0:
            normalize()
        along_x(m, Q_PART, z)
        for s in range(lines - 1):
            for line in (z - 1 - s, z + 1 + s):
                along_x(m, Q_PART, line, jnp.logical_and(line >= 0, line < lines))
        whole_out(m).start()

        @pl.loop(0, width // tile)
        def _(i):
            here = pl.ds(pl.multiple_of(i * tile, tile), tile)
            product = jnp.dot(normed[...], held[m, :, here], preferred_element_type=jnp.float32)
            if m == 0:
                gate[:, here] = product
            else:
                g = gate[:, here]
                hidden[:, here] = (g / (1.0 + jnp.exp(-g)) * product).astype(jnp.bfloat16)

    def share_copy(line, slot, sem_index):
        return pltpu.make_async_remote_copy(
            src_ref=part.at[line], dst_ref=parts_in.at[slot], send_sem=rs_send.at[line], recv_sem=rs_recv.at[sem_index],
            device_id={"fs": me_fs, "tp": line}, device_id_type=MESH,
        )

    group = cols * depth

    def group_out(line):
        here = pl.ds(pl.multiple_of(line * group, group), group)
        return pltpu.make_async_copy(held.at[2, here, :], outs[2].at[here, :], out_sem.at[2 + line])

    def mix(line, cond):
        @pl.when(cond)
        def _():
            group_out(line).start()

            @pl.loop(0, group // tile)
            def _(i):
                here = pl.ds(pl.multiple_of(line * group + i * tile, tile), tile)
                product = lax.dot_general(
                    hidden[...], held[2, here, :], (((1,), (1,)), ((), ())), preferred_element_type=jnp.float32
                )
                part[line, :, pl.ds(pl.multiple_of(i * tile, tile), tile)] = product.astype(jnp.bfloat16)

            @pl.when(line != me)
            def _():
                share_copy(line, me, me).start()

    first_half(2)
    along_x(2, Q_PART, z)
    mix(z, z >= 0)
    for s in range(lines - 1):
        along_z(2, P_PART, s, range(cols))
        for line in (z - 1 - s, z + 1 + s):
            there = jnp.logical_and(line >= 0, line < lines)
            along_x(2, Q_PART, line, there)
            mix(line, there)

    for peer in peers:
        share_copy(peer, peer, peer).wait_recv()
    step = 128

    @pl.loop(0, rows // step)
    def _(i):
        here = pl.ds(pl.multiple_of(i * step, step), step)
        total = part[me, here, :].astype(jnp.float32)
        for peer in peers:
            total = total + parts_in[peer, here, :].astype(jnp.float32)
        gate[here, 0:block] = total
        line = jnp.broadcast_to(jnp.sum(total * total, axis=1, keepdims=True), (step, 128))
        squares[:, here] = jnp.transpose(line)[0:8, :]

    def square_copy(j):
        return pltpu.make_async_remote_copy(
            src_ref=squares, dst_ref=squares_in.at[j], send_sem=sq_send.at[j], recv_sem=sq_recv.at[j],
            device_id={"fs": me_fs, "tp": peers[j]}, device_id_type=MESH,
        )

    for j in range(tp - 1):
        square_copy(j).start()
    for j in range(tp - 1):
        square_copy(j).wait_recv()
    gains = post_gain[0:1, :]

    @pl.loop(0, rows // step)
    def _(i):
        here = pl.ds(pl.multiple_of(i * step, step), step)
        total = squares[:, here]
        for j in range(tp - 1):
            total = total + squares_in[j, :, here]
        total = jnp.broadcast_to(total[0:1, :], (128, step))
        scale = lax.rsqrt(jnp.transpose(total)[:, 0:1] / (tp * block) + EPS)
        result[here, :] = (gate[here, 0:block] * scale * gains).astype(jnp.bfloat16)

    for finish in finals:
        finish()
    for j in range(tp - 1):
        token_copy(j).wait_send()
        square_copy(j).wait_send()
        share_copy(peers[j], me, me).wait_send()
    for m in range(2):
        whole_out(m).wait()
    for line in range(lines):
        group_out(line).wait()


def solution(mesh):
    fs, tp = mesh.shape["fs"], mesh.shape["tp"]
    lines, cols = tp, fs // tp

    def shards(tokens, pre_gain, gate_weight, up_weight, down_weight, post_gain):
        depth, width = gate_weight.shape
        rows, block = tokens.shape
        gate_own = (pre_gain[:, None] * gate_weight).astype(jnp.bfloat16)
        up_own = (pre_gain[:, None] * up_weight).astype(jnp.bfloat16)
        down_own = down_weight.astype(jnp.bfloat16)
        first_rows = split_rows(depth, lines, cols)
        any_space = pl.BlockSpec(memory_space=pl.ANY)
        vmem = pl.BlockSpec(memory_space=pltpu.VMEM)
        dma = pltpu.SemaphoreType.DMA
        ready = jax.ShapeDtypeStruct((fs * depth, width), jnp.bfloat16)
        return pl.pallas_call(
            functools.partial(kernel, fs, tp, lines, cols, first_rows),
            out_shape=(jax.ShapeDtypeStruct((rows, block), jnp.bfloat16), ready, ready, ready),
            in_specs=[any_space] * 4 + [vmem],
            out_specs=(vmem, any_space, any_space, any_space),
            scratch_shapes=[
                pltpu.VMEM((3, fs * depth, width), jnp.bfloat16),
                pltpu.VMEM((tp, rows, block), jnp.bfloat16),
                pltpu.VMEM((rows, tp * block), jnp.bfloat16),
                pltpu.VMEM((rows, max(width, block)), jnp.float32),
                pltpu.VMEM((rows, width), jnp.bfloat16),
                pltpu.VMEM((tp, rows, block), jnp.bfloat16),
                pltpu.VMEM((tp, rows, block), jnp.bfloat16),
                pltpu.VMEM((8, rows), jnp.float32),
                pltpu.VMEM((tp - 1, 8, rows), jnp.float32),
                dma((3, 2, fs, 4)), dma((3, 2, fs)), dma((3,)), dma((2 + lines,)),
                dma((tp - 1,)), dma((tp - 1,)), dma,
                dma((tp,)), dma((tp,)), dma((tp - 1,)), dma((tp - 1,)),
            ],
            compiler_params=pltpu.CompilerParams(collective_id=0, has_side_effects=True, vmem_limit_bytes=60 * 1024 * 1024),
        )(tokens, gate_own, up_own, down_own, post_gain[None, :])

    return jax.shard_map(
        shards,
        mesh=mesh,
        in_specs=(P("fs", "tp"), P("fs"), P("fs", "tp"), P("fs", "tp"), P("fs", "tp"), P("tp")),
        out_specs=(P("fs", "tp"), P(None, "tp"), P(None, "tp"), P(None, "tp")),
        check_vma=False,
    )
```

```python
import functools

import jax
import jax.numpy as jnp
from jax import lax
from jax.experimental import pallas as pl
from jax.experimental.pallas import tpu as pltpu
from jax.sharding import PartitionSpec as P

EPS = 1e-06
MESH = pl.DeviceIdType.MESH
P_PART, Q_PART = 0, 1
UP, DOWN, RIGHT, LEFT = 0, 1, 2, 3


def kernel(
    fs, tp, lines, cols,
    tokens, pre_gain, gate_weight, up_weight, down_weight, post_gain,
    result, gate_out, up_out, down_out,
    staged, gains_in, whole, normed, gate, hidden, part, parts_in, squares, squares_in,
    send_sem, recv_sem, stage_sem, tok_send, tok_recv, tok_own,
    rs_send, rs_recv, sq_send, sq_recv,
):
    weights, outs = (gate_weight, up_weight, down_weight), (gate_out, up_out, down_out)
    depth, width = gate_weight.shape
    half = depth // 2
    rows, block = tokens.shape
    me_fs, me = lax.axis_index("fs"), lax.axis_index("tp")
    z, x = me_fs // cols, lax.rem(me_fs, cols)
    finals = []

    sides = {
        UP: (z < lines - 1, me_fs + cols),
        DOWN: (z > 0, me_fs - cols),
        RIGHT: (x < cols - 1, me_fs + 1),
        LEFT: (x > 0, me_fs - 1),
    }
    peers = [lax.rem(me + j, tp) for j in range(1, tp)]

    def piece(m, which, shard):
        if m < 2:
            return outs[m].at[pl.ds(pl.multiple_of(shard * depth, 16), depth), :]
        return outs[2].at[pl.ds(pl.multiple_of(shard * depth + which * half, 16), half), :]

    def describe(m, which, shard, side, target):
        ref = piece(m, which, shard)
        return pltpu.make_async_remote_copy(
            src_ref=ref, dst_ref=ref,
            send_sem=send_sem.at[m, which, shard, side],
            recv_sem=recv_sem.at[m, which, shard],
            device_id={"fs": target, "tp": me}, device_id_type=MESH,
        )

    def send(m, which, shard, side, extra=None):
        there, target = sides[side]
        cond = there if extra is None else jnp.logical_and(there, extra)

        @pl.when(cond)
        def _():
            describe(m, which, shard, side, target).start()

        def finish():
            @pl.when(cond)
            def _():
                describe(m, which, shard, side, target).wait_send()

        finals.append(finish)

    def arrive(m, which, shard, cond):
        @pl.when(cond)
        def _():
            describe(m, which, shard, 0, lax.rem(me_fs + 1, fs)).wait_recv()

    barrier = pltpu.get_barrier_semaphore()
    for side in sides:
        there, target = sides[side]

        @pl.when(there)
        def _():
            pl.semaphore_signal(barrier, inc=1, device_id={"fs": target, "tp": me}, device_id_type=MESH)

    for peer in peers:
        pl.semaphore_signal(barrier, inc=1, device_id={"fs": me_fs, "tp": peer}, device_id_type=MESH)

    stages = [pltpu.make_async_copy(weights[m], staged.at[m], stage_sem.at[m]) for m in range(3)]
    for c in stages:
        c.start()
    own_tokens = pltpu.make_async_copy(tokens, whole.at[me], tok_own)
    own_tokens.start()
    gains_in[...] = jnp.transpose(jnp.broadcast_to(pre_gain[0:1, :], (128, depth)))

    def cast(m):
        stages[m].wait()

        @pl.loop(0, depth // 16)
        def _(i):
            here = pl.ds(pl.multiple_of(i * 16, 16), 16)
            v = staged[m, here, :]
            if m < 2:
                v = gains_in[here, 0:1] * v
            outs[m][pl.ds(pl.multiple_of(me_fs * depth + i * 16, 16), 16), :] = v.astype(jnp.bfloat16)

    def token_copy(j):
        return pltpu.make_async_remote_copy(
            src_ref=tokens, dst_ref=whole.at[me], send_sem=tok_send.at[j], recv_sem=tok_recv.at[j],
            device_id={"fs": me_fs, "tp": peers[j]}, device_id_type=MESH,
        )

    def start_own(m):
        for side in (UP, DOWN, RIGHT, LEFT):
            send(m, Q_PART, me_fs, side)

    cast(0)
    pl.semaphore_wait(barrier, tp - 1 + sum(there.astype(jnp.int32) for there, _ in sides.values()))
    start_own(0)
    for j in range(tp - 1):
        token_copy(j).start()
    cast(1)
    cast(2)

    def normalize():
        own_tokens.wait()
        for j in range(tp - 1):
            token_copy(j).wait_recv()
        step = 64

        @pl.loop(0, rows // step)
        def _(i):
            here = pl.ds(pl.multiple_of(i * step, step), step)
            total = jnp.zeros((step, 1), jnp.float32)
            for t in range(tp):
                v = whole[t, here, :].astype(jnp.float32)
                total = total + jnp.sum(v * v, axis=1, keepdims=True)
            scale = lax.rsqrt(total / (tp * block) + EPS)
            for t in range(tp):
                v = whole[t, here, :].astype(jnp.float32)
                normed[here, t * block:(t + 1) * block] = (v * scale).astype(jnp.bfloat16)

    def along_x(m, which, line, cond=None):
        for r in range(cols - 1):
            for side, column in ((RIGHT, x - 1 - r), (LEFT, x + 1 + r)):
                there = jnp.logical_and(column >= 0, column < cols)
                if cond is not None:
                    there = jnp.logical_and(there, cond)
                arrive(m, which, line * cols + column, there)
                if r < cols - 2:
                    send(m, which, line * cols + column, side, there)

    def valid(line):
        return jnp.logical_and(line >= 0, line < lines)

    def along_z(m, which, s, columns):
        for side, line in ((UP, z - 1 - s), (DOWN, z + 1 + s)):
            there = valid(line)
            for column in columns:
                shard = line * cols + column
                arrive(m, which, shard, there)
                if s < lines - 2:
                    send(m, which, shard, side, there)
                if which == Q_PART:
                    send(m, which, shard, RIGHT, there)
                    send(m, which, shard, LEFT, there)

    tile = 256

    def project(m):
        along_x(m, Q_PART, z)
        for s in range(lines - 1):
            for line in (z - 1 - s, z + 1 + s):
                along_x(m, Q_PART, line, valid(line))

        @pl.loop(0, width // tile)
        def _(i):
            here = pl.ds(pl.multiple_of(i * tile, tile), tile)
            product = jnp.dot(normed[...], outs[m][:, here], preferred_element_type=jnp.float32)
            if m == 0:
                gate[:, here] = product
            else:
                g = gate[:, here]
                hidden[:, here] = (g / (1.0 + jnp.exp(-g)) * product).astype(jnp.bfloat16)

    early = max(0, lines - 3)
    for s in range(lines - 1):
        along_z(0, Q_PART, s, [x])
        if s == early:
            start_own(1)
            for side in (RIGHT, LEFT):
                send(2, P_PART, me_fs, side)
    normalize()
    for s in range(lines - 1):
        along_z(1, Q_PART, s, [x])
        if s == 0:
            project(0)
        if s == early:
            start_own(2)
            along_x(2, P_PART, z)
            for column in range(cols):
                for side in (UP, DOWN):
                    send(2, P_PART, z * cols + column, side)

    def share_copy(line, sender, column, which):
        return pltpu.make_async_remote_copy(
            src_ref=part.at[line, column, which], dst_ref=parts_in.at[sender, column, which],
            send_sem=rs_send.at[line, column, which], recv_sem=rs_recv.at[sender, column, which],
            device_id={"fs": me_fs, "tp": line}, device_id_type=MESH,
        )

    def mix(line, column, which):
        here = pl.ds(pl.multiple_of((line * cols + column) * depth + which * half, 16), half)
        product = lax.dot_general(
            hidden[...], outs[2][here, :], (((1,), (1,)), ((), ())), preferred_element_type=jnp.float32
        )
        part[line, column, which] = product.astype(jnp.bfloat16)

        @pl.when(line != me)
        def _():
            share_copy(line, me, column, which).start()

    def mix_both(s, column, which):
        @pl.loop(0, 2)
        def _(i):
            line = z + (1 + s) * (2 * i - 1)

            @pl.when(valid(line))
            def _():
                mix(line, column, which)

    def others(action):
        for j in range(1, cols):
            action(lax.rem(x + j, cols))

    def near(s):
        mix_both(s, x, Q_PART)

        @pl.loop(0, cols)
        def _(c):
            mix_both(s, lax.rem(x + c, cols), P_PART)

    def far(s):
        for line in (z - 1 - s, z + 1 + s):
            along_x(2, Q_PART, line, valid(line))
        others(lambda column: mix_both(s, column, Q_PART))

    for s in range(lines - 1):
        along_z(2, Q_PART, s, [x])
        along_z(2, P_PART, s, range(cols))
        if s == 0:
            project(1)
            mix(z, x, Q_PART)

            @pl.loop(0, cols)
            def _(c):
                mix(z, lax.rem(x + c, cols), P_PART)
        near(s)
        if s == 0:
            along_x(2, Q_PART, z)
            others(lambda column: mix(z, column, Q_PART))
        else:
            far(s - 1)
    far(lines - 2)

    for peer in peers:
        for column in range(cols):
            for which in range(2):
                share_copy(peer, peer, column, which).wait_recv()
    step = 128

    @pl.loop(0, rows // step)
    def _(i):
        here = pl.ds(pl.multiple_of(i * step, step), step)
        square = jnp.zeros((step, 1), jnp.float32)
        for column in range(cols):
            for which in range(2):
                start = column * depth + which * half
                total = part[me, column, which, here, :].astype(jnp.float32)
                for peer in peers:
                    total = total + parts_in[peer, column, which, here, :].astype(jnp.float32)
                gate[here, start:start + half] = total
                square = square + jnp.sum(total * total, axis=1, keepdims=True)
        squares[:, here] = jnp.transpose(jnp.broadcast_to(square, (step, 128)))[0:8, :]

    def square_copy(j):
        return pltpu.make_async_remote_copy(
            src_ref=squares, dst_ref=squares_in.at[j], send_sem=sq_send.at[j], recv_sem=sq_recv.at[j],
            device_id={"fs": me_fs, "tp": peers[j]}, device_id_type=MESH,
        )

    for j in range(tp - 1):
        square_copy(j).start()
    for finish in finals:
        finish()
    for j in range(tp - 1):
        token_copy(j).wait_send()
        for column in range(cols):
            for which in range(2):
                share_copy(peers[j], me, column, which).wait_send()
    for j in range(tp - 1):
        square_copy(j).wait_recv()
    gains = post_gain[0:1, :]

    @pl.loop(0, rows // step)
    def _(i):
        here = pl.ds(pl.multiple_of(i * step, step), step)
        total = squares[:, here]
        for j in range(tp - 1):
            total = total + squares_in[j, :, here]
        total = jnp.broadcast_to(total[0:1, :], (128, step))
        scale = lax.rsqrt(jnp.transpose(total)[:, 0:1] / (tp * block) + EPS)
        result[here, :] = (gate[here, 0:block] * scale * gains).astype(jnp.bfloat16)

    for j in range(tp - 1):
        square_copy(j).wait_send()


def write_out(*refs):
    count = (len(refs) - 1) // 2
    copies = [pltpu.make_async_copy(refs[k], refs[count + k], refs[-1].at[k]) for k in range(count)]
    for c in copies:
        c.start()
    for c in copies:
        c.wait()


def solution(mesh):
    fs, tp = mesh.shape["fs"], mesh.shape["tp"]
    lines, cols = tp, fs // tp

    def shards(tokens, pre_gain, gate_weight, up_weight, down_weight, post_gain):
        depth, width = gate_weight.shape
        rows, block = tokens.shape
        hbm = pl.BlockSpec(memory_space=pltpu.HBM)
        vmem = pl.BlockSpec(memory_space=pltpu.VMEM)
        dma = pltpu.SemaphoreType.DMA
        half = depth // 2
        shapes = [(rows, block)] + [(fs * depth, width)] * 3
        held = pl.pallas_call(
            functools.partial(kernel, fs, tp, lines, cols),
            out_shape=tuple(pltpu.VMEM(s, jnp.bfloat16) for s in shapes),
            in_specs=[hbm, vmem, hbm, hbm, hbm, vmem],
            out_specs=(vmem,) * 4,
            scratch_shapes=[
                pltpu.VMEM((3, depth, width), jnp.float32),
                pltpu.VMEM((depth, 128), jnp.float32),
                pltpu.VMEM((tp, rows, block), jnp.bfloat16),
                pltpu.VMEM((rows, tp * block), jnp.bfloat16),
                pltpu.VMEM((rows, max(width, block)), jnp.float32),
                pltpu.VMEM((rows, width), jnp.bfloat16),
                pltpu.VMEM((tp, cols, 2, rows, half), jnp.bfloat16),
                pltpu.VMEM((tp, cols, 2, rows, half), jnp.bfloat16),
                pltpu.VMEM((8, rows), jnp.float32),
                pltpu.VMEM((tp - 1, 8, rows), jnp.float32),
                dma((3, 2, fs, 4)), dma((3, 2, fs)), dma((3,)),
                dma((tp - 1,)), dma((tp - 1,)), dma,
                dma((tp, cols, 2)), dma((tp, cols, 2)), dma((tp - 1,)), dma((tp - 1,)),
            ],
            compiler_params=pltpu.CompilerParams(collective_id=0, has_side_effects=True, vmem_limit_bytes=42 * 1024 * 1024),
        )(tokens, pre_gain[None, :], gate_weight, up_weight, down_weight, post_gain[None, :])
        return tuple(pl.pallas_call(
            write_out,
            out_shape=tuple(jax.ShapeDtypeStruct(s, jnp.bfloat16) for s in shapes),
            in_specs=[vmem] * 4,
            out_specs=(hbm,) * 4,
            scratch_shapes=[dma((4,))],
            compiler_params=pltpu.CompilerParams(vmem_limit_bytes=1024 * 1024),
        )(*held))

    return jax.shard_map(
        shards,
        mesh=mesh,
        in_specs=(P("fs", "tp"), P("fs"), P("fs", "tp"), P("fs", "tp"), P("fs", "tp"), P("tp")),
        out_specs=(P("fs", "tp"), P(None, "tp"), P(None, "tp"), P(None, "tp")),
        check_vma=False,
    )
```

```python
import functools

import jax
import jax.numpy as jnp
from jax import lax
from jax.experimental import pallas as pl
from jax.experimental.pallas import tpu as pltpu
from jax.sharding import PartitionSpec as P

EPS = 1e-06
MESH = pl.DeviceIdType.MESH
P_PART, Q_PART = 0, 1
UP, DOWN, RIGHT, LEFT = 0, 1, 2, 3


def kernel(
    fs, tp, lines, cols,
    tokens, pre_gain, gate_weight, up_weight, down_weight, post_gain,
    result, gate_out, up_out, down_out,
    staged, gains_in, whole, normed, gate, hidden, part, parts_in, squares, squares_in,
    send_sem, recv_sem, stage_sem, tok_send, tok_recv, tok_own,
    rs_send, rs_recv, sq_send, sq_recv,
):
    weights, outs = (gate_weight, up_weight, down_weight), (gate_out, up_out, down_out)
    depth, width = gate_weight.shape
    half = depth // 2
    rows, block = tokens.shape
    me_fs, me = lax.axis_index("fs"), lax.axis_index("tp")
    z, x = me_fs // cols, lax.rem(me_fs, cols)
    finals = []

    sides = {
        UP: (z < lines - 1, me_fs + cols),
        DOWN: (z > 0, me_fs - cols),
        RIGHT: (x < cols - 1, me_fs + 1),
        LEFT: (x > 0, me_fs - 1),
    }
    peers = [lax.rem(me + j, tp) for j in range(1, tp)]

    def piece(m, which, shard):
        if m < 2:
            return outs[m].at[pl.ds(pl.multiple_of(shard * depth, 16), depth), :]
        return outs[2].at[pl.ds(pl.multiple_of(shard * depth + which * half, 16), half), :]

    def describe(m, which, shard, side, target):
        ref = piece(m, which, shard)
        return pltpu.make_async_remote_copy(
            src_ref=ref, dst_ref=ref,
            send_sem=send_sem.at[m, which, shard, side],
            recv_sem=recv_sem.at[m, which, shard],
            device_id={"fs": target, "tp": me}, device_id_type=MESH,
        )

    def send(m, which, shard, side, extra=None):
        there, target = sides[side]
        cond = there if extra is None else jnp.logical_and(there, extra)

        @pl.when(cond)
        def _():
            describe(m, which, shard, side, target).start()

        def finish():
            @pl.when(cond)
            def _():
                describe(m, which, shard, side, target).wait_send()

        finals.append(finish)

    def arrive(m, which, shard, cond):
        @pl.when(cond)
        def _():
            describe(m, which, shard, 0, lax.rem(me_fs + 1, fs)).wait_recv()

    barrier = pltpu.get_barrier_semaphore()
    for side in sides:
        there, target = sides[side]

        @pl.when(there)
        def _():
            pl.semaphore_signal(barrier, inc=1, device_id={"fs": target, "tp": me}, device_id_type=MESH)

    for peer in peers:
        pl.semaphore_signal(barrier, inc=1, device_id={"fs": me_fs, "tp": peer}, device_id_type=MESH)

    stages = [pltpu.make_async_copy(weights[m], staged.at[m], stage_sem.at[m]) for m in range(3)]
    for c in stages:
        c.start()
    own_tokens = pltpu.make_async_copy(tokens, whole.at[me], tok_own)
    own_tokens.start()
    gains_in[...] = jnp.transpose(jnp.broadcast_to(pre_gain[0:1, :], (128, depth)))

    def cast(m):
        stages[m].wait()

        @pl.loop(0, depth // 16)
        def _(i):
            here = pl.ds(pl.multiple_of(i * 16, 16), 16)
            v = staged[m, here, :]
            if m < 2:
                v = gains_in[here, 0:1] * v
            outs[m][pl.ds(pl.multiple_of(me_fs * depth + i * 16, 16), 16), :] = v.astype(jnp.bfloat16)

    def token_copy(j):
        return pltpu.make_async_remote_copy(
            src_ref=tokens, dst_ref=whole.at[me], send_sem=tok_send.at[j], recv_sem=tok_recv.at[j],
            device_id={"fs": me_fs, "tp": peers[j]}, device_id_type=MESH,
        )

    def start_own(m):
        for side in (UP, DOWN, RIGHT, LEFT):
            send(m, Q_PART, me_fs, side)

    cast(0)
    pl.semaphore_wait(barrier, tp - 1 + sum(there.astype(jnp.int32) for there, _ in sides.values()))
    start_own(0)
    for j in range(tp - 1):
        token_copy(j).start()
    cast(1)
    cast(2)

    def normalize():
        own_tokens.wait()
        for j in range(tp - 1):
            token_copy(j).wait_recv()
        step = 64

        @pl.loop(0, rows // step)
        def _(i):
            here = pl.ds(pl.multiple_of(i * step, step), step)
            total = jnp.zeros((step, 1), jnp.float32)
            for t in range(tp):
                v = whole[t, here, :].astype(jnp.float32)
                total = total + jnp.sum(v * v, axis=1, keepdims=True)
            scale = lax.rsqrt(total / (tp * block) + EPS)
            for t in range(tp):
                v = whole[t, here, :].astype(jnp.float32)
                normed[here, t * block:(t + 1) * block] = (v * scale).astype(jnp.bfloat16)

    def along_x(m, which, line, cond=None):
        for r in range(cols - 1):
            for side, column in ((RIGHT, x - 1 - r), (LEFT, x + 1 + r)):
                there = jnp.logical_and(column >= 0, column < cols)
                if cond is not None:
                    there = jnp.logical_and(there, cond)
                arrive(m, which, line * cols + column, there)
                if r < cols - 2:
                    send(m, which, line * cols + column, side, there)

    def valid(line):
        return jnp.logical_and(line >= 0, line < lines)

    def along_z(m, which, s, columns, cond=None):
        for side, line in ((UP, z - 1 - s), (DOWN, z + 1 + s)):
            there = valid(line) if cond is None else jnp.logical_and(valid(line), cond)
            for column in columns:
                shard = line * cols + column
                arrive(m, which, shard, there)
                if s < lines - 2:
                    send(m, which, shard, side, there)
                if which == Q_PART:
                    send(m, which, shard, RIGHT, there)
                    send(m, which, shard, LEFT, there)

    tile = 256

    def project(m):
        along_x(m, Q_PART, z)
        for s in range(lines - 1):
            for line in (z - 1 - s, z + 1 + s):
                along_x(m, Q_PART, line, valid(line))

        @pl.loop(0, width // tile)
        def _(i):
            here = pl.ds(pl.multiple_of(i * tile, tile), tile)
            product = jnp.dot(normed[...], outs[m][:, here], preferred_element_type=jnp.float32)
            if m == 0:
                gate[:, here] = product
            else:
                g = gate[:, here]
                hidden[:, here] = (g / (1.0 + jnp.exp(-g)) * product).astype(jnp.bfloat16)

    early = max(0, lines - 3)
    for s in range(lines - 1):
        along_z(0, Q_PART, s, [x])
        if s == early:
            start_own(1)
            for side in (RIGHT, LEFT):
                send(2, P_PART, me_fs, side)
    normalize()
    for s in range(lines - 1):
        along_z(1, Q_PART, s, [x])
        if s == early:
            start_own(2)
            along_x(2, P_PART, z)
            for column in range(cols):
                for side in (UP, DOWN):
                    send(2, P_PART, z * cols + column, side)
            project(0)

    def share_copy(line, sender, column, which):
        return pltpu.make_async_remote_copy(
            src_ref=part.at[line, column, which], dst_ref=parts_in.at[sender, column, which],
            send_sem=rs_send.at[line, column, which], recv_sem=rs_recv.at[sender, column, which],
            device_id={"fs": me_fs, "tp": line}, device_id_type=MESH,
        )

    def mix(line, column, which):
        here = pl.ds(pl.multiple_of((line * cols + column) * depth + which * half, 16), half)
        product = lax.dot_general(
            hidden[...], outs[2][here, :], (((1,), (1,)), ((), ())), preferred_element_type=jnp.float32
        )
        part[line, column, which] = product.astype(jnp.bfloat16)

        @pl.when(line != me)
        def _():
            share_copy(line, me, column, which).start()

    def mix_both(s, column, which):
        @pl.loop(0, 2)
        def _(i):
            line = z + (1 + s) * (2 * i - 1)

            @pl.when(valid(line))
            def _():
                mix(line, column, which)

    def others(action):
        for j in range(1, cols):
            action(lax.rem(x + j, cols))

    def near(s):
        mix_both(s, x, Q_PART)

        @pl.loop(0, cols)
        def _(c):
            mix_both(s, lax.rem(x + c, cols), P_PART)

    def far(s):
        for line in (z - 1 - s, z + 1 + s):
            along_x(2, Q_PART, line, valid(line))
        others(lambda column: mix_both(s, column, Q_PART))

    inner = jnp.logical_and(z > 0, z < lines - 1)

    def down_step(s, cond=None):
        along_z(2, Q_PART, s, [x], cond)
        along_z(2, P_PART, s, range(cols), cond)

    down_step(0)
    for s in range(1, lines - 2):
        down_step(s, inner)
    project(1)
    mix(z, x, Q_PART)

    @pl.loop(0, cols)
    def _(c):
        mix(z, lax.rem(x + c, cols), P_PART)

    if lines > 2:
        near(0)
    for s in range(1, lines - 2):
        down_step(s, jnp.logical_not(inner))
        if s == 1:
            along_x(2, Q_PART, z)
            others(lambda column: mix(z, column, Q_PART))
        near(s)
        far(s - 1)
    last = lines - 2
    if last > 0:
        along_z(2, Q_PART, last, [x])
        mix_both(last, x, Q_PART)
    else:
        mix_both(last, x, Q_PART)
    if last < 2:
        along_x(2, Q_PART, z)
        others(lambda column: mix(z, column, Q_PART))
    if last > 0:
        far(last - 1)
    for column in range(cols):
        if last > 0:
            along_z(2, P_PART, last, [column])
        mix_both(last, column, P_PART)
    far(last)

    for peer in peers:
        for column in range(cols):
            for which in range(2):
                share_copy(peer, peer, column, which).wait_recv()
    step = 128

    @pl.loop(0, rows // step)
    def _(i):
        here = pl.ds(pl.multiple_of(i * step, step), step)
        square = jnp.zeros((step, 1), jnp.float32)
        for column in range(cols):
            for which in range(2):
                start = column * depth + which * half
                total = part[me, column, which, here, :].astype(jnp.float32)
                for peer in peers:
                    total = total + parts_in[peer, column, which, here, :].astype(jnp.float32)
                gate[here, start:start + half] = total
                square = square + jnp.sum(total * total, axis=1, keepdims=True)
        squares[:, here] = jnp.transpose(jnp.broadcast_to(square, (step, 128)))[0:8, :]

    def square_copy(j):
        return pltpu.make_async_remote_copy(
            src_ref=squares, dst_ref=squares_in.at[j], send_sem=sq_send.at[j], recv_sem=sq_recv.at[j],
            device_id={"fs": me_fs, "tp": peers[j]}, device_id_type=MESH,
        )

    for j in range(tp - 1):
        square_copy(j).start()
    for finish in finals:
        finish()
    for j in range(tp - 1):
        token_copy(j).wait_send()
        for column in range(cols):
            for which in range(2):
                share_copy(peers[j], me, column, which).wait_send()
    for j in range(tp - 1):
        square_copy(j).wait_recv()
    gains = post_gain[0:1, :]

    @pl.loop(0, rows // step)
    def _(i):
        here = pl.ds(pl.multiple_of(i * step, step), step)
        total = squares[:, here]
        for j in range(tp - 1):
            total = total + squares_in[j, :, here]
        total = jnp.broadcast_to(total[0:1, :], (128, step))
        scale = lax.rsqrt(jnp.transpose(total)[:, 0:1] / (tp * block) + EPS)
        result[here, :] = (gate[here, 0:block] * scale * gains).astype(jnp.bfloat16)

    for j in range(tp - 1):
        square_copy(j).wait_send()


def write_out(*refs):
    count = (len(refs) - 1) // 2
    copies = [pltpu.make_async_copy(refs[k], refs[count + k], refs[-1].at[k]) for k in range(count)]
    for c in copies:
        c.start()
    for c in copies:
        c.wait()


def solution(mesh):
    fs, tp = mesh.shape["fs"], mesh.shape["tp"]
    lines, cols = tp, fs // tp

    def shards(tokens, pre_gain, gate_weight, up_weight, down_weight, post_gain):
        depth, width = gate_weight.shape
        rows, block = tokens.shape
        hbm = pl.BlockSpec(memory_space=pltpu.HBM)
        vmem = pl.BlockSpec(memory_space=pltpu.VMEM)
        dma = pltpu.SemaphoreType.DMA
        half = depth // 2
        shapes = [(rows, block)] + [(fs * depth, width)] * 3
        held = pl.pallas_call(
            functools.partial(kernel, fs, tp, lines, cols),
            out_shape=tuple(pltpu.VMEM(s, jnp.bfloat16) for s in shapes),
            in_specs=[hbm, vmem, hbm, hbm, hbm, vmem],
            out_specs=(vmem,) * 4,
            scratch_shapes=[
                pltpu.VMEM((3, depth, width), jnp.float32),
                pltpu.VMEM((depth, 128), jnp.float32),
                pltpu.VMEM((tp, rows, block), jnp.bfloat16),
                pltpu.VMEM((rows, tp * block), jnp.bfloat16),
                pltpu.VMEM((rows, max(width, block)), jnp.float32),
                pltpu.VMEM((rows, width), jnp.bfloat16),
                pltpu.VMEM((tp, cols, 2, rows, half), jnp.bfloat16),
                pltpu.VMEM((tp, cols, 2, rows, half), jnp.bfloat16),
                pltpu.VMEM((8, rows), jnp.float32),
                pltpu.VMEM((tp - 1, 8, rows), jnp.float32),
                dma((3, 2, fs, 4)), dma((3, 2, fs)), dma((3,)),
                dma((tp - 1,)), dma((tp - 1,)), dma,
                dma((tp, cols, 2)), dma((tp, cols, 2)), dma((tp - 1,)), dma((tp - 1,)),
            ],
            compiler_params=pltpu.CompilerParams(collective_id=0, has_side_effects=True, vmem_limit_bytes=42 * 1024 * 1024),
        )(tokens, pre_gain[None, :], gate_weight, up_weight, down_weight, post_gain[None, :])
        return tuple(pl.pallas_call(
            write_out,
            out_shape=tuple(jax.ShapeDtypeStruct(s, jnp.bfloat16) for s in shapes),
            in_specs=[vmem] * 4,
            out_specs=(hbm,) * 4,
            scratch_shapes=[dma((4,))],
            compiler_params=pltpu.CompilerParams(vmem_limit_bytes=1024 * 1024),
        )(*held))

    return jax.shard_map(
        shards,
        mesh=mesh,
        in_specs=(P("fs", "tp"), P("fs"), P("fs", "tp"), P("fs", "tp"), P("fs", "tp"), P("tp")),
        out_specs=(P("fs", "tp"), P(None, "tp"), P(None, "tp"), P(None, "tp")),
        check_vma=False,
    )
```

```python
import functools

import jax
import jax.numpy as jnp
from jax import lax
from jax.experimental import pallas as pl
from jax.experimental.pallas import tpu as pltpu
from jax.sharding import PartitionSpec as P

EPS = 1e-06
MESH = pl.DeviceIdType.MESH
P_PART, Q_PART = 0, 1
UP, DOWN, RIGHT, LEFT = 0, 1, 2, 3
CHUNKS = 4


def kernel(
    fs, tp, lines, cols,
    tokens, pre_gain, gate_weight, up_weight, down_weight, post_gain,
    result, gate_out, up_out, down_out,
    staged, gains_in, whole, normed, gate, hidden, part, parts_in, squares, squares_in,
    send_sem, recv_sem, stage_sem, tok_send, tok_recv, tok_own,
    rs_send, rs_recv, sq_send, sq_recv,
):
    weights, outs = (gate_weight, up_weight, down_weight), (gate_out, up_out, down_out)
    depth, width = gate_weight.shape
    half = depth // 2
    rows, block = tokens.shape
    me_fs, me = lax.axis_index("fs"), lax.axis_index("tp")
    z, x = me_fs // cols, lax.rem(me_fs, cols)
    finals = []

    sides = {
        UP: (z < lines - 1, me_fs + cols),
        DOWN: (z > 0, me_fs - cols),
        RIGHT: (x < cols - 1, me_fs + 1),
        LEFT: (x > 0, me_fs - 1),
    }
    peers = [lax.rem(me + j, tp) for j in range(1, tp)]

    def piece(m, which, shard):
        if m < 2:
            return outs[m].at[pl.ds(pl.multiple_of(shard * depth, 16), depth), :]
        return outs[2].at[pl.ds(pl.multiple_of(shard * depth + which * half, 16), half), :]

    def describe(m, which, shard, side, target):
        ref = piece(m, which, shard)
        return pltpu.make_async_remote_copy(
            src_ref=ref, dst_ref=ref,
            send_sem=send_sem.at[m, which, shard, side],
            recv_sem=recv_sem.at[m, which, shard],
            device_id={"fs": target, "tp": me}, device_id_type=MESH,
        )

    def send(m, which, shard, side, extra=None):
        there, target = sides[side]
        cond = there if extra is None else jnp.logical_and(there, extra)

        @pl.when(cond)
        def _():
            describe(m, which, shard, side, target).start()

        def finish():
            @pl.when(cond)
            def _():
                describe(m, which, shard, side, target).wait_send()

        finals.append(finish)

    def arrive(m, which, shard, cond):
        @pl.when(cond)
        def _():
            describe(m, which, shard, 0, lax.rem(me_fs + 1, fs)).wait_recv()

    barrier = pltpu.get_barrier_semaphore()
    for side in sides:
        there, target = sides[side]

        @pl.when(there)
        def _():
            pl.semaphore_signal(barrier, inc=1, device_id={"fs": target, "tp": me}, device_id_type=MESH)

    for peer in peers:
        pl.semaphore_signal(barrier, inc=1, device_id={"fs": me_fs, "tp": peer}, device_id_type=MESH)

    stages = [pltpu.make_async_copy(weights[m], staged.at[m], stage_sem.at[m]) for m in range(3)]
    for c in stages:
        c.start()
    own_tokens = pltpu.make_async_copy(tokens, whole.at[me], tok_own)
    own_tokens.start()
    gains_in[...] = jnp.transpose(jnp.broadcast_to(pre_gain[0:1, :], (128, depth)))

    def cast(m):
        stages[m].wait()

        @pl.loop(0, depth // 16)
        def _(i):
            here = pl.ds(pl.multiple_of(i * 16, 16), 16)
            v = staged[m, here, :]
            if m < 2:
                v = gains_in[here, 0:1] * v
            outs[m][pl.ds(pl.multiple_of(me_fs * depth + i * 16, 16), 16), :] = v.astype(jnp.bfloat16)

    def token_copy(j):
        return pltpu.make_async_remote_copy(
            src_ref=tokens, dst_ref=whole.at[me], send_sem=tok_send.at[j], recv_sem=tok_recv.at[j],
            device_id={"fs": me_fs, "tp": peers[j]}, device_id_type=MESH,
        )

    def start_own(m, which_sides=(UP, DOWN, RIGHT, LEFT)):
        for side in which_sides:
            send(m, Q_PART, me_fs, side)

    cast(0)
    pl.semaphore_wait(barrier, tp - 1 + sum(there.astype(jnp.int32) for there, _ in sides.values()))
    start_own(0)
    for j in range(tp - 1):
        token_copy(j).start()
    cast(1)
    cast(2)

    def normalize():
        own_tokens.wait()
        for j in range(tp - 1):
            token_copy(j).wait_recv()
        step = 64

        @pl.loop(0, rows // step)
        def _(i):
            here = pl.ds(pl.multiple_of(i * step, step), step)
            total = jnp.zeros((step, 1), jnp.float32)
            for t in range(tp):
                v = whole[t, here, :].astype(jnp.float32)
                total = total + jnp.sum(v * v, axis=1, keepdims=True)
            scale = lax.rsqrt(total / (tp * block) + EPS)
            for t in range(tp):
                v = whole[t, here, :].astype(jnp.float32)
                normed[here, t * block:(t + 1) * block] = (v * scale).astype(jnp.bfloat16)

    def along_x(m, which, line, cond=None):
        for r in range(cols - 1):
            for side, column in ((RIGHT, x - 1 - r), (LEFT, x + 1 + r)):
                there = jnp.logical_and(column >= 0, column < cols)
                if cond is not None:
                    there = jnp.logical_and(there, cond)
                arrive(m, which, line * cols + column, there)
                if r < cols - 2:
                    send(m, which, line * cols + column, side, there)

    def valid(line):
        return jnp.logical_and(line >= 0, line < lines)

    def along_z(m, which, s, columns, cond=None):
        for side, line in ((UP, z - 1 - s), (DOWN, z + 1 + s)):
            there = valid(line) if cond is None else jnp.logical_and(valid(line), cond)
            for column in columns:
                shard = line * cols + column
                arrive(m, which, shard, there)
                if s < lines - 2:
                    send(m, which, shard, side, there)
                if which == Q_PART:
                    send(m, which, shard, RIGHT, there)
                    send(m, which, shard, LEFT, there)

    tile = 256

    def project(m):
        along_x(m, Q_PART, z)
        for s in range(lines - 1):
            for line in (z - 1 - s, z + 1 + s):
                along_x(m, Q_PART, line, valid(line))

        @pl.loop(0, width // tile)
        def _(i):
            here = pl.ds(pl.multiple_of(i * tile, tile), tile)
            product = jnp.dot(normed[...], outs[m][:, here], preferred_element_type=jnp.float32)
            if m == 0:
                gate[:, here] = product
            else:
                g = gate[:, here]
                hidden[:, here] = (g / (1.0 + jnp.exp(-g)) * product).astype(jnp.bfloat16)

    early = max(0, lines - 3)
    for s in range(lines - 1):
        along_z(0, Q_PART, s, [x])
        if s == early:
            start_own(1)
            for side in (RIGHT, LEFT):
                send(2, P_PART, me_fs, side)
    normalize()
    for s in range(lines - 1):
        along_z(1, Q_PART, s, [x])
        if s == early:
            start_own(2, (UP, DOWN))
            along_x(2, P_PART, z)
            for column in range(cols):
                for side in (UP, DOWN):
                    send(2, P_PART, z * cols + column, side)
            project(0)
    start_own(2, (RIGHT, LEFT))

    def share_copy(line, sender, column, which):
        return pltpu.make_async_remote_copy(
            src_ref=part.at[line, column, which], dst_ref=parts_in.at[sender, column, which],
            send_sem=rs_send.at[line, column, which], recv_sem=rs_recv.at[sender, column, which],
            device_id={"fs": me_fs, "tp": line}, device_id_type=MESH,
        )

    def mix(line, column, which):
        here = pl.ds(pl.multiple_of((line * cols + column) * depth + which * half, 16), half)
        product = lax.dot_general(
            hidden[...], outs[2][here, :], (((1,), (1,)), ((), ())), preferred_element_type=jnp.float32
        )
        part[line, column, which] = product.astype(jnp.bfloat16)

        @pl.when(line != me)
        def _():
            share_copy(line, me, column, which).start()

    def mix_both(s, column, which):
        @pl.loop(0, 2)
        def _(i):
            line = z + (1 + s) * (2 * i - 1)

            @pl.when(valid(line))
            def _():
                mix(line, column, which)

    def others(action):
        for j in range(1, cols):
            action(lax.rem(x + j, cols))

    def near(s):
        mix_both(s, x, Q_PART)

        @pl.loop(0, cols)
        def _(c):
            mix_both(s, lax.rem(x + c, cols), P_PART)

    def far(s):
        for line in (z - 1 - s, z + 1 + s):
            along_x(2, Q_PART, line, valid(line))
        others(lambda column: mix_both(s, column, Q_PART))

    inner = jnp.logical_and(z > 0, z < lines - 1)

    def down_step(s, cond=None):
        along_z(2, Q_PART, s, [x], cond)
        along_z(2, P_PART, s, range(cols), cond)

    down_step(0)
    for s in range(1, lines - 2):
        down_step(s, inner)
    project(1)
    mix(z, x, Q_PART)

    @pl.loop(0, cols)
    def _(c):
        mix(z, lax.rem(x + c, cols), P_PART)

    if lines > 2:
        near(0)
    for s in range(1, lines - 2):
        down_step(s, jnp.logical_not(inner))
        if s == 1:
            along_x(2, Q_PART, z)
            others(lambda column: mix(z, column, Q_PART))
        near(s)
        far(s - 1)
    last = lines - 2
    if last > 0:
        along_z(2, Q_PART, last, [x])
        mix_both(last, x, Q_PART)
    else:
        mix_both(last, x, Q_PART)
    if last < 2:
        along_x(2, Q_PART, z)
        others(lambda column: mix(z, column, Q_PART))
    if last > 0:
        far(last - 1)
    for column in range(cols):
        if last > 0:
            along_z(2, P_PART, last, [column])
        mix_both(last, column, P_PART)
    far(last)

    for peer in peers:
        for column in range(cols):
            for which in range(2):
                share_copy(peer, peer, column, which).wait_recv()
    step = 128

    @pl.loop(0, rows // step)
    def _(i):
        here = pl.ds(pl.multiple_of(i * step, step), step)
        square = jnp.zeros((step, 1), jnp.float32)
        for column in range(cols):
            for which in range(2):
                start = column * depth + which * half
                total = part[me, column, which, here, :].astype(jnp.float32)
                for peer in peers:
                    total = total + parts_in[peer, column, which, here, :].astype(jnp.float32)
                gate[here, start:start + half] = total
                square = square + jnp.sum(total * total, axis=1, keepdims=True)
        squares[:, here] = jnp.transpose(jnp.broadcast_to(square, (step, 128)))[0:8, :]

    def square_copy(j):
        return pltpu.make_async_remote_copy(
            src_ref=squares, dst_ref=squares_in.at[j], send_sem=sq_send.at[j], recv_sem=sq_recv.at[j],
            device_id={"fs": me_fs, "tp": peers[j]}, device_id_type=MESH,
        )

    for j in range(tp - 1):
        square_copy(j).start()
    for finish in finals:
        finish()
    for j in range(tp - 1):
        token_copy(j).wait_send()
        for column in range(cols):
            for which in range(2):
                share_copy(peers[j], me, column, which).wait_send()
    for j in range(tp - 1):
        square_copy(j).wait_recv()
    gains = post_gain[0:1, :]

    @pl.loop(0, rows // step)
    def _(i):
        here = pl.ds(pl.multiple_of(i * step, step), step)
        total = squares[:, here]
        for j in range(tp - 1):
            total = total + squares_in[j, :, here]
        total = jnp.broadcast_to(total[0:1, :], (128, step))
        scale = lax.rsqrt(jnp.transpose(total)[:, 0:1] / (tp * block) + EPS)
        result[here, :] = (gate[here, 0:block] * scale * gains).astype(jnp.bfloat16)

    for j in range(tp - 1):
        square_copy(j).wait_send()


def write_out(*refs):
    count = (len(refs) - 1) // 2
    copies = []
    for k in range(count):
        size = refs[k].shape[0] // CHUNKS
        for c in range(CHUNKS):
            here = pl.ds(c * size, size)
            copies.append(pltpu.make_async_copy(refs[k].at[here, :], refs[count + k].at[here, :], refs[-1].at[k, c]))
    for c in copies:
        c.start()
    for c in copies:
        c.wait()


def solution(mesh):
    fs, tp = mesh.shape["fs"], mesh.shape["tp"]
    lines, cols = tp, fs // tp

    def shards(tokens, pre_gain, gate_weight, up_weight, down_weight, post_gain):
        depth, width = gate_weight.shape
        rows, block = tokens.shape
        hbm = pl.BlockSpec(memory_space=pltpu.HBM)
        vmem = pl.BlockSpec(memory_space=pltpu.VMEM)
        dma = pltpu.SemaphoreType.DMA
        half = depth // 2
        shapes = [(rows, block)] + [(fs * depth, width)] * 3
        held = pl.pallas_call(
            functools.partial(kernel, fs, tp, lines, cols),
            out_shape=tuple(pltpu.VMEM(s, jnp.bfloat16) for s in shapes),
            in_specs=[hbm, vmem, hbm, hbm, hbm, vmem],
            out_specs=(vmem,) * 4,
            scratch_shapes=[
                pltpu.VMEM((3, depth, width), jnp.float32),
                pltpu.VMEM((depth, 128), jnp.float32),
                pltpu.VMEM((tp, rows, block), jnp.bfloat16),
                pltpu.VMEM((rows, tp * block), jnp.bfloat16),
                pltpu.VMEM((rows, max(width, block)), jnp.float32),
                pltpu.VMEM((rows, width), jnp.bfloat16),
                pltpu.VMEM((tp, cols, 2, rows, half), jnp.bfloat16),
                pltpu.VMEM((tp, cols, 2, rows, half), jnp.bfloat16),
                pltpu.VMEM((8, rows), jnp.float32),
                pltpu.VMEM((tp - 1, 8, rows), jnp.float32),
                dma((3, 2, fs, 4)), dma((3, 2, fs)), dma((3,)),
                dma((tp - 1,)), dma((tp - 1,)), dma,
                dma((tp, cols, 2)), dma((tp, cols, 2)), dma((tp - 1,)), dma((tp - 1,)),
            ],
            compiler_params=pltpu.CompilerParams(collective_id=0, has_side_effects=True, vmem_limit_bytes=42 * 1024 * 1024),
        )(tokens, pre_gain[None, :], gate_weight, up_weight, down_weight, post_gain[None, :])
        return tuple(pl.pallas_call(
            write_out,
            out_shape=tuple(jax.ShapeDtypeStruct(s, jnp.bfloat16) for s in shapes),
            in_specs=[vmem] * 4,
            out_specs=(hbm,) * 4,
            scratch_shapes=[dma((4, CHUNKS))],
            compiler_params=pltpu.CompilerParams(vmem_limit_bytes=1024 * 1024),
        )(*held))

    return jax.shard_map(
        shards,
        mesh=mesh,
        in_specs=(P("fs", "tp"), P("fs"), P("fs", "tp"), P("fs", "tp"), P("fs", "tp"), P("tp")),
        out_specs=(P("fs", "tp"), P(None, "tp"), P(None, "tp"), P(None, "tp")),
        check_vma=False,
    )
```

```python
import functools

import jax
import jax.numpy as jnp
from jax import lax
from jax.experimental import pallas as pl
from jax.experimental.pallas import tpu as pltpu
from jax.sharding import PartitionSpec as P

EPS = 1e-06
MESH = pl.DeviceIdType.MESH
P_PART, Q_PART = 0, 1
UP, DOWN, RIGHT, LEFT = 0, 1, 2, 3
CHUNKS = 4


def kernel(
    fs, tp, lines, cols,
    tokens, pre_gain, gate_weight, up_weight, down_weight,
    gate, squares, squares_in, gate_out, up_out, down_out,
    staged, gains_in, whole, normed, hidden, part, parts_in,
    send_sem, recv_sem, stage_sem, tok_send, tok_recv, tok_own,
    rs_send, rs_recv, sq_send, sq_recv,
):
    weights, outs = (gate_weight, up_weight, down_weight), (gate_out, up_out, down_out)
    depth, width = gate_weight.shape
    half = depth // 2
    rows, block = tokens.shape
    me_fs, me = lax.axis_index("fs"), lax.axis_index("tp")
    z, x = me_fs // cols, lax.rem(me_fs, cols)
    finals = []

    sides = {
        UP: (z < lines - 1, me_fs + cols),
        DOWN: (z > 0, me_fs - cols),
        RIGHT: (x < cols - 1, me_fs + 1),
        LEFT: (x > 0, me_fs - 1),
    }
    peers = [lax.rem(me + j, tp) for j in range(1, tp)]

    def piece(m, which, shard):
        if m < 2:
            return outs[m].at[pl.ds(pl.multiple_of(shard * depth, 16), depth), :]
        return outs[2].at[pl.ds(pl.multiple_of(shard * depth + which * half, 16), half), :]

    def describe(m, which, shard, side, target):
        ref = piece(m, which, shard)
        return pltpu.make_async_remote_copy(
            src_ref=ref, dst_ref=ref,
            send_sem=send_sem.at[m, which, shard, side],
            recv_sem=recv_sem.at[m, which, shard],
            device_id={"fs": target, "tp": me}, device_id_type=MESH,
        )

    def send(m, which, shard, side, extra=None):
        there, target = sides[side]
        cond = there if extra is None else jnp.logical_and(there, extra)

        @pl.when(cond)
        def _():
            describe(m, which, shard, side, target).start()

        def finish():
            @pl.when(cond)
            def _():
                describe(m, which, shard, side, target).wait_send()

        finals.append(finish)

    def arrive(m, which, shard, cond):
        @pl.when(cond)
        def _():
            describe(m, which, shard, 0, lax.rem(me_fs + 1, fs)).wait_recv()

    barrier = pltpu.get_barrier_semaphore()
    for side in sides:
        there, target = sides[side]

        @pl.when(there)
        def _():
            pl.semaphore_signal(barrier, inc=1, device_id={"fs": target, "tp": me}, device_id_type=MESH)

    for peer in peers:
        pl.semaphore_signal(barrier, inc=1, device_id={"fs": me_fs, "tp": peer}, device_id_type=MESH)

    stages = [pltpu.make_async_copy(weights[m], staged.at[m], stage_sem.at[m]) for m in range(3)]
    for c in stages:
        c.start()
    own_tokens = pltpu.make_async_copy(tokens, whole.at[me], tok_own)
    own_tokens.start()
    gains_in[...] = jnp.transpose(jnp.broadcast_to(pre_gain[0:1, :], (128, depth)))

    def cast(m):
        stages[m].wait()

        @pl.loop(0, depth // 16)
        def _(i):
            here = pl.ds(pl.multiple_of(i * 16, 16), 16)
            v = staged[m, here, :]
            if m < 2:
                v = gains_in[here, 0:1] * v
            outs[m][pl.ds(pl.multiple_of(me_fs * depth + i * 16, 16), 16), :] = v.astype(jnp.bfloat16)

    def token_copy(j):
        return pltpu.make_async_remote_copy(
            src_ref=tokens, dst_ref=whole.at[me], send_sem=tok_send.at[j], recv_sem=tok_recv.at[j],
            device_id={"fs": me_fs, "tp": peers[j]}, device_id_type=MESH,
        )

    def start_own(m, which_sides=(UP, DOWN, RIGHT, LEFT)):
        for side in which_sides:
            send(m, Q_PART, me_fs, side)

    cast(0)
    pl.semaphore_wait(barrier, tp - 1 + sum(there.astype(jnp.int32) for there, _ in sides.values()))
    start_own(0)
    for j in range(tp - 1):
        token_copy(j).start()
    cast(1)
    cast(2)

    def normalize():
        own_tokens.wait()
        for j in range(tp - 1):
            token_copy(j).wait_recv()
        step = 64

        @pl.loop(0, rows // step)
        def _(i):
            here = pl.ds(pl.multiple_of(i * step, step), step)
            total = jnp.zeros((step, 1), jnp.float32)
            for t in range(tp):
                v = whole[t, here, :].astype(jnp.float32)
                total = total + jnp.sum(v * v, axis=1, keepdims=True)
            scale = lax.rsqrt(total / (tp * block) + EPS)
            for t in range(tp):
                v = whole[t, here, :].astype(jnp.float32)
                normed[here, t * block:(t + 1) * block] = (v * scale).astype(jnp.bfloat16)

    def along_x(m, which, line, cond=None):
        for r in range(cols - 1):
            for side, column in ((RIGHT, x - 1 - r), (LEFT, x + 1 + r)):
                there = jnp.logical_and(column >= 0, column < cols)
                if cond is not None:
                    there = jnp.logical_and(there, cond)
                arrive(m, which, line * cols + column, there)
                if r < cols - 2:
                    send(m, which, line * cols + column, side, there)

    def valid(line):
        return jnp.logical_and(line >= 0, line < lines)

    def along_z(m, which, s, columns, cond=None):
        for side, line in ((UP, z - 1 - s), (DOWN, z + 1 + s)):
            there = valid(line) if cond is None else jnp.logical_and(valid(line), cond)
            for column in columns:
                shard = line * cols + column
                arrive(m, which, shard, there)
                if s < lines - 2:
                    send(m, which, shard, side, there)
                if which == Q_PART:
                    send(m, which, shard, RIGHT, there)
                    send(m, which, shard, LEFT, there)

    tile = 256

    def project(m):
        along_x(m, Q_PART, z)
        for s in range(lines - 1):
            for line in (z - 1 - s, z + 1 + s):
                along_x(m, Q_PART, line, valid(line))

        @pl.loop(0, width // tile)
        def _(i):
            here = pl.ds(pl.multiple_of(i * tile, tile), tile)
            product = jnp.dot(normed[...], outs[m][:, here], preferred_element_type=jnp.float32)
            if m == 0:
                gate[:, here] = product
            else:
                g = gate[:, here]
                hidden[:, here] = (g / (1.0 + jnp.exp(-g)) * product).astype(jnp.bfloat16)

    early = max(0, lines - 3)
    for s in range(lines - 1):
        along_z(0, Q_PART, s, [x])
        if s == early:
            start_own(1)
            for side in (RIGHT, LEFT):
                send(2, P_PART, me_fs, side)
    normalize()
    for s in range(lines - 1):
        along_z(1, Q_PART, s, [x])
        if s == early:
            start_own(2, (UP, DOWN))
            along_x(2, P_PART, z)
            for column in range(cols):
                for side in (UP, DOWN):
                    send(2, P_PART, z * cols + column, side)
            project(0)
    start_own(2, (RIGHT, LEFT))

    def share_copy(line, sender, column, which):
        return pltpu.make_async_remote_copy(
            src_ref=part.at[line, column, which], dst_ref=parts_in.at[sender, column, which],
            send_sem=rs_send.at[line, column, which], recv_sem=rs_recv.at[sender, column, which],
            device_id={"fs": me_fs, "tp": line}, device_id_type=MESH,
        )

    def mix(line, column, which):
        here = pl.ds(pl.multiple_of((line * cols + column) * depth + which * half, 16), half)
        product = lax.dot_general(
            hidden[...], outs[2][here, :], (((1,), (1,)), ((), ())), preferred_element_type=jnp.float32
        )
        part[line, column, which] = product.astype(jnp.bfloat16)

        @pl.when(line != me)
        def _():
            share_copy(line, me, column, which).start()

    def mix_both(s, column, which):
        @pl.loop(0, 2)
        def _(i):
            line = z + (1 + s) * (2 * i - 1)

            @pl.when(valid(line))
            def _():
                mix(line, column, which)

    def others(action):
        for j in range(1, cols):
            action(lax.rem(x + j, cols))

    def near(s):
        mix_both(s, x, Q_PART)

        @pl.loop(0, cols)
        def _(c):
            mix_both(s, lax.rem(x + c, cols), P_PART)

    def far(s):
        for line in (z - 1 - s, z + 1 + s):
            along_x(2, Q_PART, line, valid(line))
        others(lambda column: mix_both(s, column, Q_PART))

    inner = jnp.logical_and(z > 0, z < lines - 1)

    def down_step(s, cond=None):
        along_z(2, Q_PART, s, [x], cond)
        along_z(2, P_PART, s, range(cols), cond)

    down_step(0)
    for s in range(1, lines - 2):
        down_step(s, inner)
    project(1)
    mix(z, x, Q_PART)

    @pl.loop(0, cols)
    def _(c):
        mix(z, lax.rem(x + c, cols), P_PART)

    if lines > 2:
        near(0)
    for s in range(1, lines - 2):
        down_step(s, jnp.logical_not(inner))
        if s == 1:
            along_x(2, Q_PART, z)
            others(lambda column: mix(z, column, Q_PART))
        near(s)
        far(s - 1)
    last = lines - 2
    if last > 0:
        along_z(2, Q_PART, last, [x])
        mix_both(last, x, Q_PART)
    else:
        mix_both(last, x, Q_PART)
    if last < 2:
        along_x(2, Q_PART, z)
        others(lambda column: mix(z, column, Q_PART))
    if last > 0:
        far(last - 1)
    for column in range(cols):
        if last > 0:
            along_z(2, P_PART, last, [column])
        mix_both(last, column, P_PART)
    far(last)

    for peer in peers:
        for column in range(cols):
            for which in range(2):
                share_copy(peer, peer, column, which).wait_recv()
    step = 128

    @pl.loop(0, rows // step)
    def _(i):
        here = pl.ds(pl.multiple_of(i * step, step), step)
        square = jnp.zeros((step, 1), jnp.float32)
        for column in range(cols):
            for which in range(2):
                start = column * depth + which * half
                total = part[me, column, which, here, :].astype(jnp.float32)
                for peer in peers:
                    total = total + parts_in[peer, column, which, here, :].astype(jnp.float32)
                gate[here, start:start + half] = total
                square = square + jnp.sum(total * total, axis=1, keepdims=True)
        squares[:, here] = jnp.transpose(jnp.broadcast_to(square, (step, 128)))[0:8, :]

    def square_copy(j):
        return pltpu.make_async_remote_copy(
            src_ref=squares, dst_ref=squares_in.at[j], send_sem=sq_send.at[j], recv_sem=sq_recv.at[j],
            device_id={"fs": me_fs, "tp": peers[j]}, device_id_type=MESH,
        )

    for j in range(tp - 1):
        square_copy(j).start()
    for finish in finals:
        finish()
    for j in range(tp - 1):
        token_copy(j).wait_send()
        for column in range(cols):
            for which in range(2):
                share_copy(peers[j], me, column, which).wait_send()
    for j in range(tp - 1):
        square_copy(j).wait_recv()
    for j in range(tp - 1):
        square_copy(j).wait_send()


def write_out(
    width, share, squares, squares_in, gate_held, up_held, down_held, post_gain,
    result_out, gate_out, up_out, down_out, result, sems, last,
):
    copies = []
    for k, (ref, out) in enumerate(((gate_held, gate_out), (up_held, up_out), (down_held, down_out))):
        size = ref.shape[0] // CHUNKS
        for c in range(CHUNKS):
            here = pl.ds(c * size, size)
            copies.append(pltpu.make_async_copy(ref.at[here, :], out.at[here, :], sems.at[k, c]))
    for c in copies:
        c.start()
    rows, block = result.shape
    gains = post_gain[0:1, :]
    step = 128

    @pl.loop(0, rows // step)
    def _(i):
        here = pl.ds(pl.multiple_of(i * step, step), step)
        total = squares[:, here]
        for j in range(squares_in.shape[0]):
            total = total + squares_in[j, :, here]
        total = jnp.broadcast_to(total[0:1, :], (128, step))
        scale = lax.rsqrt(jnp.transpose(total)[:, 0:1] / width + EPS)
        result[here, :] = (share[here, 0:block] * scale * gains).astype(jnp.bfloat16)

    final = pltpu.make_async_copy(result, result_out, last)
    final.start()
    for c in copies:
        c.wait()
    final.wait()


def solution(mesh):
    fs, tp = mesh.shape["fs"], mesh.shape["tp"]
    lines, cols = tp, fs // tp

    def shards(tokens, pre_gain, gate_weight, up_weight, down_weight, post_gain):
        depth, width = gate_weight.shape
        rows, block = tokens.shape
        hbm = pl.BlockSpec(memory_space=pltpu.HBM)
        vmem = pl.BlockSpec(memory_space=pltpu.VMEM)
        dma = pltpu.SemaphoreType.DMA
        half = depth // 2
        shapes = [(rows, block)] + [(fs * depth, width)] * 3
        held = pl.pallas_call(
            functools.partial(kernel, fs, tp, lines, cols),
            out_shape=(
                pltpu.VMEM((rows, max(width, block)), jnp.float32),
                pltpu.VMEM((8, rows), jnp.float32),
                pltpu.VMEM((tp - 1, 8, rows), jnp.float32),
            ) + tuple(pltpu.VMEM(s, jnp.bfloat16) for s in shapes[1:]),
            in_specs=[hbm, vmem, hbm, hbm, hbm],
            out_specs=(vmem,) * 6,
            scratch_shapes=[
                pltpu.VMEM((3, depth, width), jnp.float32),
                pltpu.VMEM((depth, 128), jnp.float32),
                pltpu.VMEM((tp, rows, block), jnp.bfloat16),
                pltpu.VMEM((rows, tp * block), jnp.bfloat16),
                pltpu.VMEM((rows, width), jnp.bfloat16),
                pltpu.VMEM((tp, cols, 2, rows, half), jnp.bfloat16),
                pltpu.VMEM((tp, cols, 2, rows, half), jnp.bfloat16),
                dma((3, 2, fs, 4)), dma((3, 2, fs)), dma((3,)),
                dma((tp - 1,)), dma((tp - 1,)), dma,
                dma((tp, cols, 2)), dma((tp, cols, 2)), dma((tp - 1,)), dma((tp - 1,)),
            ],
            compiler_params=pltpu.CompilerParams(collective_id=0, has_side_effects=True, vmem_limit_bytes=38 * 1024 * 1024),
        )(tokens, pre_gain[None, :], gate_weight, up_weight, down_weight)
        return tuple(pl.pallas_call(
            functools.partial(write_out, tp * block),
            out_shape=tuple(jax.ShapeDtypeStruct(s, jnp.bfloat16) for s in shapes),
            in_specs=[vmem] * 7,
            out_specs=(hbm,) * 4,
            scratch_shapes=[pltpu.VMEM((rows, block), jnp.bfloat16), dma((3, CHUNKS)), dma],
            compiler_params=pltpu.CompilerParams(vmem_limit_bytes=2 * 1024 * 1024),
        )(*held, post_gain[None, :]))

    return jax.shard_map(
        shards,
        mesh=mesh,
        in_specs=(P("fs", "tp"), P("fs"), P("fs", "tp"), P("fs", "tp"), P("fs", "tp"), P("tp")),
        out_specs=(P("fs", "tp"), P(None, "tp"), P(None, "tp"), P(None, "tp")),
        check_vma=False,
    )
```
